32 devices in a mesh: ep: 16 (over z, x, core), tp: 2 (over y).
Axes of the slice: x: 2, y: 2, z: 4, core: 2. Of those that a mesh axis runs over, the one named last changes fastest.
Arguments:
- tokens: bfloat16 [192, 1024], P('ep'), may hold values from -6 to 6
- norm_gain: float32 [1024], replicated, may hold values from 0.1 to 1.9
- w_query: bfloat16 [1024, 512], P(None, 'tp'), may hold values from -0.1875 to 0.1875
- w_key: bfloat16 [1024, 512], P(None, 'tp'), may hold values from -0.1875 to 0.1875
- w_value: bfloat16 [1024, 512], P(None, 'tp'), may hold values from -0.1875 to 0.1875
- w_input_gate: bfloat16 [1024, 4], replicated, may hold values from -0.1875 to 0.1875
- w_forget_gate: bfloat16 [1024, 4], replicated, may hold values from -0.1875 to 0.1875
- input_bias: float32 [4], replicated, may hold values from -2 to 1
- forget_bias: float32 [4], replicated, may hold values from 0 to 4
- state_c: float32 [192, 4, 128, 128], P('ep', 'tp'), may hold values from -1.75 to 1.75
- state_n: float32 [192, 4, 128], P('ep', 'tp'), may hold values from -1.75 to 1.75
- state_m: float32 [192, 4], P('ep', 'tp'), may hold values from -1 to 2
- w_mixer_out: bfloat16 [512, 1024], P('tp'), may hold values from -0.25 to 0.25
- ffn_gain: float32 [1024], replicated, may hold values from 0.1 to 1.9
- routes: int32 [192, 6], P('ep'), may hold values from 0 to 15, all different within a row; in each aligned block of 12 rows (0 to 11, 12 to 23, ...) at most 10 rows name the same one
- route_scale: bfloat16 [192, 6], P('ep'), may hold values from 0.099609375 to 1
- w_expert_gate: bfloat16 [16, 1024, 1024], P('ep', None, 'tp'), may hold values from -0.375 to 0.375
- w_expert_up: bfloat16 [16, 1024, 1024], P('ep', None, 'tp'), may hold values from -0.375 to 0.375
- w_expert_down: bfloat16 [16, 1024, 1024], P('ep', 'tp'), may hold values from -0.1875 to 0.1875
- w_dense_gate: bfloat16 [1024, 512], P(None, 'tp'), may hold values from -0.1875 to 0.1875
- w_dense_up: bfloat16 [1024, 512], P(None, 'tp'), may hold values from -0.1875 to 0.1875
- w_dense_down: bfloat16 [512, 1024], P('tp'), may hold values from -0.5 to 0.5
- w_branch_gate: bfloat16 [1024], replicated, may hold values from -0.1875 to 0.1875
Outputs:
- output: bfloat16 [192, 1024], P('ep', 'tp')
- new_c: float32 [192, 4, 128, 128], P('ep', 'tp')
- new_n: float32 [192, 4, 128], P('ep', 'tp')
- new_m: float32 [192, 4], P('ep', 'tp')
The draws below stay inside these ranges and needn't reach their ends.
Inputs may be any that keep to these rules, and one draw needn't show every extreme that they name: `routes`: each row names 6 different experts. Among the rows of one index of ep no expert is named by more than 10 rows, a bound that some block reaches of them.
All inputs are finite; a program needn't handle non-finite values.
Results may differ from the reference program's by a relative error of at most 0.018.
Values may be sent and summed in bfloat16 or wider, within the bound.
A program may use at most 64 MiB of HBM per device.

```python
import math
import jax
import jax.numpy as jnp
import numpy as np
from jax import lax

D = 1024
HEADS = 4
DQK = 128
DV = 128
D_EXPERT = 1024
DENSE_FF = 512
TOP_K = 6
SEQ_DEV = 12
EXPERTS = 16
TOKENS = 192
CAP = 10
N_TP = 2


def block_scale(rng, dims, split, low, top_value):
    gain = 1.0
    for dim, parts in split:
        draws = jax.random.uniform(jax.random.fold_in(jax.random.fold_in(rng, 6), dim), (parts,), jnp.float32, low / len(split), top_value / len(split))
        gain = gain * jnp.repeat(jnp.exp(draws), dims[dim] // parts).reshape((-1,) + (1,) * (len(dims) - 1 - dim))
    return gain


def assign_block(rng, own, number, rows, count, top, most, slope):
    sequence = jax.random.permutation(rng, count)
    crowded, common = shares(count, rows * top, most, slope, True), shares(count, rows * top, most, slope, False)
    places = jnp.arange(count)

    def named(sizes, turn):
        used = int((sizes > 0).sum())
        fixed = max(1, used // 4)
        moved = fixed + (places - fixed + turn * (used - fixed)) % max(1, count - fixed)
        return jnp.zeros((count,), jnp.int32).at[sequence[jnp.where(places < fixed, places, moved)]].set(jnp.asarray(sizes, jnp.int32))

    sizes = jnp.where(number % 4 == 0, named(crowded, number // 4), named(common, number - number // 4 - 1))
    mixed = jax.random.permutation(jax.random.fold_in(own, 3), count)
    donor, taker = mixed[0:count // 2 * 2:2], mixed[1:count // 2 * 2:2]
    room = jnp.minimum(sizes[donor] - 1, most - sizes[taker]) // 2
    room = jnp.where((donor == sequence[0]) | (taker == sequence[0]) | (sizes[taker] == 0), 0, jnp.maximum(room, 0))
    moved = jax.random.randint(jax.random.fold_in(own, 4), (count // 2,), 0, 1 << 20) % (room + 1)
    sizes = sizes.at[donor].add(-moved).at[taker].add(moved)
    members = jnp.searchsorted(jnp.cumsum(sizes), jnp.arange(rows * top), side="right").astype(jnp.int32)
    listing = members.reshape(top, rows).T
    listing = listing[jax.random.permutation(jax.random.fold_in(own, 1), rows)]
    turn = jax.random.randint(jax.random.fold_in(own, 2), (rows, 1), 0, top)
    return jnp.take_along_axis(listing, (jnp.arange(top)[None, :] + turn) % top, axis=1)


def shares(number_of, total, most, lean, full):
    weights = [(1 << 20) // math.isqrt(standing ** lean) + 1 for standing in range(1, number_of + 1)]
    largest = most if full else min(most, max(-(-total // number_of), total * weights[0] // sum(weights)))
    least = 1 if total - largest >= number_of - 1 else 0
    given, surplus = [largest] + [least] * (number_of - 1), total - largest - least * (number_of - 1)
    while surplus > 0:
        free = [i for i in range(1, number_of) if given[i] < largest] or [i for i in range(1, number_of) if given[i] < most]
        whole, left = sum([weights[i] for i in free]), surplus
        for i in free:
            extra = min(most - given[i], max(1, left * weights[i] // whole), surplus)
            given[i] = given[i] + extra
            surplus = surplus - extra
    return np.array(given)


def scatter_about(own_key, shape, spread, limit, pieces=(), kind=jnp.bfloat16):
    array = jax.random.normal(own_key, shape, jnp.float32) * spread
    if len(pieces) > 0:
        array = block_scale(own_key, shape, pieces, -0.22, 0.18) * array
    return jnp.clip(array, min=-limit, max=limit).astype(kind)


def setup_inputs(seed: int = 0) -> dict:
    key_list = jax.random.split(jax.random.key(seed), 24)
    tokens = scatter_about(key_list[0], (TOKENS, D), 1.0, 6.0, ((0, 16),))
    norm_gain = jnp.clip(1.0 + 0.18 * jax.random.normal(key_list[1], (D,), jnp.float32), 0.1, 1.9)
    w_query = scatter_about(key_list[2], (D, HEADS * DQK), D ** -0.5, 0.1875, ((1, 2),))
    w_key = scatter_about(key_list[3], (D, HEADS * DQK), D ** -0.5, 0.1875, ((1, 2),))
    w_value = scatter_about(key_list[4], (D, HEADS * DV), D ** -0.5, 0.1875, ((1, 2),))
    w_input_gate = scatter_about(key_list[5], (D, HEADS), D ** -0.5, 0.1875)
    w_forget_gate = scatter_about(key_list[6], (D, HEADS), D ** -0.5, 0.1875)
    input_bias = jnp.clip(jax.random.uniform(key_list[7], (HEADS,), jnp.float32, -2.0, 1.0), -2.0, 1.0)
    forget_bias = jnp.clip(jax.random.uniform(key_list[8], (HEADS,), jnp.float32, 0.0, 4.0), 0.0, 4.0)
    state_c = scatter_about(key_list[9], (TOKENS, HEADS, DQK, DV), 0.3, 1.75, ((0, 16), (1, 2)), jnp.float32)
    state_n = scatter_about(key_list[10], (TOKENS, HEADS, DQK), 0.3, 1.75, ((0, 16), (1, 2)), jnp.float32)
    state_m = jnp.clip(-1.0 + 3.0 * jax.random.uniform(key_list[11], (TOKENS, HEADS), jnp.float32) ** block_scale(key_list[11], (TOKENS, HEADS), ((0, 16), (1, 2)), -0.2, 0.2), -1.0, 2.0)
    w_mixer_out = scatter_about(key_list[12], (HEADS * DV, D), (HEADS * DV) ** -0.5, 0.25, ((0, 2),))
    ffn_gain = jnp.clip(1.0 + 0.18 * jax.random.normal(key_list[13], (D,), jnp.float32), 0.1, 1.9)
    routes_keys = jax.random.split(jax.random.fold_in(key_list[14], 1), TOKENS // SEQ_DEV)
    routes_turns = jax.random.permutation(jax.random.fold_in(key_list[14], 3), TOKENS // SEQ_DEV)
    routes = jax.vmap(lambda own, number: assign_block(jax.random.fold_in(key_list[14], 2), own, number, SEQ_DEV, EXPERTS, TOP_K, CAP, 2))(routes_keys, routes_turns).reshape((TOKENS, TOP_K))
    route_scale = jnp.clip(jnp.exp(math.log(1.0) - 2.306499 * jax.random.uniform(key_list[15], (TOKENS, TOP_K), jnp.float32) ** block_scale(key_list[15], (TOKENS, TOP_K), ((0, 16),), -0.2, 0.2)), 0.099609375, 1.0).astype(jnp.bfloat16)
    w_expert_gate = scatter_about(key_list[16], (EXPERTS, D, D_EXPERT), (2.0 * D ** -0.5), 0.375, ((0, 16), (2, 2)))
    w_expert_up = scatter_about(key_list[17], (EXPERTS, D, D_EXPERT), (2.0 * D ** -0.5), 0.375, ((0, 16), (2, 2)))
    w_expert_down = scatter_about(key_list[18], (EXPERTS, D_EXPERT, D), D_EXPERT ** -0.5, 0.1875, ((0, 16), (1, 2)))
    w_dense_gate = scatter_about(key_list[19], (D, DENSE_FF), D ** -0.5, 0.1875, ((1, 2),))
    w_dense_up = scatter_about(key_list[20], (D, DENSE_FF), D ** -0.5, 0.1875, ((1, 2),))
    w_dense_down = scatter_about(key_list[21], (DENSE_FF, D), (DENSE_FF // 4) ** -0.5, 0.5, ((0, 2),))
    w_branch_gate = scatter_about(key_list[22], (D,), D ** -0.5, 0.1875)
    return {"tokens": tokens, "norm_gain": norm_gain, "w_query": w_query, "w_key": w_key, "w_value": w_value, "w_input_gate": w_input_gate, "w_forget_gate": w_forget_gate, "input_bias": input_bias, "forget_bias": forget_bias, "state_c": state_c, "state_n": state_n, "state_m": state_m, "w_mixer_out": w_mixer_out, "ffn_gain": ffn_gain, "routes": routes, "route_scale": route_scale, "w_expert_gate": w_expert_gate, "w_expert_up": w_expert_up, "w_expert_down": w_expert_down, "w_dense_gate": w_dense_gate, "w_dense_up": w_dense_up, "w_dense_down": w_dense_down, "w_branch_gate": w_branch_gate}


EPSILON = 1e-06
CLAMP_LIMIT = 7.0
SWISH_ALPHA = 1.702

def stored(values):
    return lax.optimization_barrier(values.astype(jnp.bfloat16)).astype(jnp.float32)

def rms_scaled(values, gain_vec):
    values = values.astype(jnp.float32)
    scaled = values * lax.rsqrt(lax.optimization_barrier(jnp.mean(values * values, axis=-1, keepdims=True)) + EPSILON)
    return scaled * gain_vec.astype(jnp.float32)

def slot_tables(route_blocks, expert_ids, weight_blocks, capacity, top_count):
    entries = route_blocks.shape[1]
    matched = (route_blocks[:, None, :] == expert_ids[None, :, None]).astype(jnp.int32)
    ranking = jnp.cumsum(matched, axis=2, dtype=jnp.int32) - 1
    slot_ids = jnp.arange(capacity, dtype=jnp.int32)
    chosen = (matched[:, :, None, :] == 1) & (ranking[:, :, None, :] == slot_ids[None, None, :, None])
    slot_hot = jnp.where(chosen, 1.0, 0.0).astype(jnp.float32)
    entry_ids = jnp.arange(entries, dtype=jnp.int32)
    token_ids = jnp.arange(entries // top_count, dtype=jnp.int32)
    owner = jnp.where(entry_ids[:, None] // top_count == token_ids[None, :], 1.0, 0.0).astype(jnp.float32)
    token_hot = jnp.einsum('becj,js->becs', slot_hot, owner, precision=lax.Precision.HIGHEST)
    slot_weight = jnp.einsum('becj,bj->bec', slot_hot, weight_blocks, precision=lax.Precision.HIGHEST)
    return (token_hot, slot_weight)

def reference(tokens, norm_gain, w_query, w_key, w_value, w_input_gate, w_forget_gate, input_bias, forget_bias, state_c, state_n, state_m, w_mixer_out, ffn_gain, routes, route_scale, w_expert_gate, w_expert_up, w_expert_down, w_dense_gate, w_dense_up, w_dense_down, w_branch_gate):
    row_count = tokens.shape[0]
    normed = rms_scaled(tokens, norm_gain).astype(jnp.bfloat16)
    queries = stored(jnp.dot(normed, w_query, preferred_element_type=jnp.float32)).reshape(row_count, HEADS, DQK)
    key_rows = stored(jnp.dot(normed, w_key, preferred_element_type=jnp.float32)).reshape(row_count, HEADS, DQK)
    value_rows = stored(jnp.dot(normed, w_value, preferred_element_type=jnp.float32)).reshape(row_count, HEADS, DV)
    input_pre = jnp.dot(normed, w_input_gate, preferred_element_type=jnp.float32) + input_bias
    forget_log = jax.nn.log_sigmoid(jnp.dot(normed, w_forget_gate, preferred_element_type=jnp.float32) + forget_bias)
    new_m = jnp.maximum(forget_log + state_m, input_pre)
    forget_factor = jnp.exp(forget_log + state_m - new_m)
    input_factor = jnp.exp(input_pre - new_m)
    key_scaled = key_rows * DQK ** (-0.5)
    new_c = forget_factor[..., None, None] * state_c + input_factor[..., None, None] * (key_scaled[..., :, None] * value_rows[..., None, :])
    new_n = forget_factor[..., None] * state_n + input_factor[..., None] * key_scaled
    numer = jnp.einsum('thd,thdv->thv', queries, new_c, precision=lax.Precision.HIGHEST)
    denom = jnp.einsum('thd,thd->th', queries, new_n, precision=lax.Precision.HIGHEST)
    head_out = (numer / jnp.maximum(jnp.abs(denom), 1.0)[..., None]).astype(jnp.bfloat16).reshape(row_count, HEADS * DV)
    group_width = HEADS // N_TP * DV
    mixer_total = jnp.zeros((row_count, D), jnp.float32)
    for group in range(N_TP):
        lower = group * group_width
        mixer_total = mixer_total + stored(jnp.dot(head_out[:, lower:lower + group_width], w_mixer_out[lower:lower + group_width], preferred_element_type=jnp.float32))
    mixer_out = mixer_total.astype(jnp.bfloat16)
    residual = tokens.astype(jnp.float32) + mixer_out.astype(jnp.float32)
    ffn_in = rms_scaled(residual, ffn_gain).astype(jnp.bfloat16)
    scale_values = route_scale.astype(jnp.float32)
    route_weight = scale_values / lax.optimization_barrier(jnp.sum(scale_values, axis=1, keepdims=True))
    block_count = row_count // SEQ_DEV
    route_blocks = routes.reshape(block_count, SEQ_DEV * TOP_K)
    weight_blocks = route_weight.reshape(block_count, SEQ_DEV * TOP_K)
    token_blocks = ffn_in.astype(jnp.float32).reshape(block_count, SEQ_DEV, D)
    part_width = D_EXPERT // N_TP

    def one_expert(total, inputs):
        gate_weight, up_weight, down_weight, expert = inputs
        token_hot, slot_weight = slot_tables(route_blocks, expert[None], weight_blocks, CAP, TOP_K)
        token_hot = token_hot[:, 0]
        slot_weight = slot_weight[:, 0]
        slot_rows = jnp.einsum('bcs,bsd->bcd', token_hot, token_blocks, precision=lax.Precision.HIGHEST).astype(jnp.bfloat16).reshape(block_count * CAP, D)
        gate_pre = jnp.minimum(jnp.dot(slot_rows, gate_weight, preferred_element_type=jnp.float32), CLAMP_LIMIT)
        up_pre = jnp.clip(jnp.dot(slot_rows, up_weight, preferred_element_type=jnp.float32), -CLAMP_LIMIT, CLAMP_LIMIT)
        hidden = (gate_pre * jax.nn.sigmoid(SWISH_ALPHA * gate_pre) * (up_pre + 1.0)).astype(jnp.bfloat16)
        expert_out = jnp.zeros((block_count * CAP, D), jnp.float32)
        for part in range(N_TP):
            lower = part * part_width
            expert_out = expert_out + stored(jnp.dot(hidden[:, lower:lower + part_width], down_weight[lower:lower + part_width], preferred_element_type=jnp.float32))
        weighted = expert_out.reshape(block_count, CAP, D) * slot_weight[..., None]
        total = total + jnp.einsum('bcs,bcd->bsd', token_hot, weighted, precision=lax.Precision.HIGHEST)
        return (total, None)
    moe, _ = lax.scan(one_expert, jnp.zeros((block_count, SEQ_DEV, D), jnp.float32), (w_expert_gate, w_expert_up, w_expert_down, jnp.arange(EXPERTS, dtype=jnp.int32)))
    dense_gate_pre = jnp.dot(ffn_in, w_dense_gate, preferred_element_type=jnp.float32)
    dense_hidden = (jax.nn.silu(dense_gate_pre) * jnp.dot(ffn_in, w_dense_up, preferred_element_type=jnp.float32)).astype(jnp.bfloat16)
    dense = jnp.dot(dense_hidden, w_dense_down, preferred_element_type=jnp.float32)
    branch_weight = jax.nn.sigmoid(jnp.dot(ffn_in, w_branch_gate, preferred_element_type=jnp.float32))
    output = (residual + moe.reshape(row_count, D) + branch_weight[:, None] * dense).astype(jnp.bfloat16)
    return (output, new_c, new_n, new_m)
```

```python
import functools

import jax
import jax.numpy as jnp
from jax import lax
from jax.experimental import pallas as pl
from jax.experimental.pallas import tpu as pltpu
from jax.sharding import PartitionSpec as P

EPSILON = 1e-06
CLAMP_LIMIT = 7.0
SWISH_ALPHA = 1.702
MESH = pl.DeviceIdType.MESH
F32 = jnp.float32
BF16 = jnp.bfloat16
VMEM_LIMIT = 60000 * 1024


def padded(values, rows):
    extra = rows - values.shape[0]
    if extra == 0:
        return values
    return jnp.concatenate([values, jnp.zeros((extra, values.shape[1]), values.dtype)], axis=0)


def dot(left, right):
    return jnp.dot(left, right, preferred_element_type=F32)


def dot_nt(left, right):
    return lax.dot_general(left, right, (((1,), (1,)), ((), ())), preferred_element_type=F32)


def rms_scaled(values, gain):
    scale = lax.rsqrt(jnp.mean(values * values, axis=-1, keepdims=True) + EPSILON)
    return values * scale * gain


def column(values, index):
    lanes = lax.broadcasted_iota(jnp.int32, values.shape, 1)
    return jnp.sum(jnp.where(lanes == index, values, 0.0), axis=1, keepdims=True)


def cell_kernel(
    tokens_ref,
    gain_ref,
    wq_ref,
    wk_ref,
    wv_ref,
    wi_ref,
    wf_ref,
    ib_ref,
    fb_ref,
    c_hbm,
    n_ref,
    m_ref,
    mix_hbm,
    part_ref,
    newc_hbm,
    newn_ref,
    newm_ref,
    c_buf,
    co_buf,
    mix_buf,
    num_buf,
    in_sem,
    out_sem,
    mix_sem,
):
    rows = tokens_ref.shape[0]
    pad_rows = part_ref.shape[0]
    heads = m_ref.shape[1]
    dk, dv = c_buf.shape[2], c_buf.shape[3]
    first = lax.axis_index("tp") * heads
    for t in range(rows):
        pltpu.make_async_copy(c_hbm.at[t], c_buf.at[t], in_sem.at[t]).start()
    pltpu.make_async_copy(mix_hbm, mix_buf, mix_sem).start()
    tokens = padded(tokens_ref[...].astype(F32), pad_rows)
    normed = rms_scaled(tokens, gain_ref[...]).astype(BF16)
    queries = dot(normed, wq_ref[...]).astype(BF16).astype(F32)
    keys = dot(normed, wk_ref[...]).astype(BF16).astype(F32)
    values = dot(normed, wv_ref[...]).astype(BF16).astype(F32)
    pre_all = dot_nt(normed, wi_ref[...]) + ib_ref[...]
    fg_all = dot_nt(normed, wf_ref[...]) + fb_ref[...]
    fg_all = jnp.minimum(fg_all, 0.0) - jnp.log(1.0 + jnp.exp(-jnp.abs(fg_all)))
    state_m = padded(m_ref[...], pad_rows)
    key_scale = dk**-0.5
    per_head = []
    for h in range(heads):
        pre = column(pre_all, first + h)
        shifted = column(fg_all, first + h) + state_m[:, h : h + 1]
        new_m = jnp.maximum(shifted, pre)
        forget = jnp.exp(shifted - new_m)
        inflow = jnp.exp(pre - new_m)
        newm_ref[:, h : h + 1] = new_m[:rows]
        q = queries[:, h * dk : (h + 1) * dk]
        k = keys[:, h * dk : (h + 1) * dk] * (inflow * key_scale)
        v = values[:, h * dv : (h + 1) * dv]
        new_n = forget * padded(n_ref[:, h, :], pad_rows) + k
        newn_ref[:, h, :] = new_n[:rows]
        denom = jnp.maximum(jnp.abs(jnp.sum(q * new_n, axis=1, keepdims=True)), 1.0)
        per_head.append((forget, q.T, k.T, v, denom))
    num_buf[...] = jnp.zeros(num_buf.shape, F32)
    for t in range(rows):
        pltpu.make_async_copy(c_hbm.at[t], c_buf.at[t], in_sem.at[t]).wait()
        for h in range(heads):
            forget, q_t, k_t, v, _ = per_head[h]
            new_c = forget[t : t + 1] * c_buf[t, h] + k_t[:, t : t + 1] * v[t : t + 1]
            co_buf[t, h] = new_c
            num_buf[t : t + 1, h * dv : (h + 1) * dv] = jnp.sum(
                q_t[:, t : t + 1] * new_c, axis=0, keepdims=True
            )
        pltpu.make_async_copy(co_buf.at[t], newc_hbm.at[t], out_sem.at[t]).start()
    head_out = jnp.concatenate(
        [num_buf[:, h * dv : (h + 1) * dv] / per_head[h][4] for h in range(heads)], axis=1
    ).astype(BF16)
    pltpu.make_async_copy(mix_hbm, mix_buf, mix_sem).wait()
    part_ref[...] = dot(head_out, mix_buf[...]).astype(BF16)
    for t in range(rows):
        pltpu.make_async_copy(co_buf.at[t], newc_hbm.at[t], out_sem.at[t]).wait()


def ffn_kernel(
    sizes,
    tokens_ref,
    part_ref,
    gain_ref,
    routes_ref,
    scale_ref,
    wb_ref,
    eg_hbm,
    eu_hbm,
    ed_hbm,
    dg_hbm,
    du_hbm,
    dd_hbm,
    out_ref,
    eg,
    eu,
    ed,
    dg,
    du,
    dd,
    mixed,
    own_w,
    blocks,
    weights,
    outs,
    from_core,
    summed,
    from_x,
    to_z,
    from_z,
    residual_buf,
    acc_buf,
    acc_send,
    from_y,
    load_sem,
    mix_s,
    mix_r,
    w_s,
    w_r,
    gz_s,
    gz_r,
    gx_s,
    gx_r,
    gc_s,
    gc_r,
    rc_s,
    rc_r,
    rx_s,
    rx_r,
    rz_s,
    rz_r,
    ry_s,
    ry_r,
):
    nz, nx, nc, ntp = sizes
    ep = lax.axis_index("ep")
    tp = lax.axis_index("tp")
    c = lax.rem(ep, nc)
    x = lax.rem(lax.div(ep, nc), nx)
    z = lax.div(ep, nc * nx)
    rows, width = tokens_ref.shape
    pad_rows = part_ref.shape[0]
    cw = width // ntp

    def at(dc, dx, dz):
        return {
            "ep": (lax.rem(z + dz + nz, nz) * nx + lax.rem(x + dx + nx, nx)) * nc
            + lax.rem(c + dc + nc, nc)
        }

    def tp_at(dy):
        return {"tp": lax.rem(tp + dy + ntp, ntp)}

    def remote(src, dst, send, recv, device):
        return pltpu.make_async_remote_copy(
            src_ref=src, dst_ref=dst, send_sem=send, recv_sem=recv, device_id=device, device_id_type=MESH
        )

    pending = []

    def send(copy):
        copy.start()
        pending.append(copy)

    others = [
        (dc, dx, dz)
        for dc in range(nc)
        for dx in range(nx)
        for dz in range(nz)
        if (dc, dx, dz) != (0, 0, 0)
    ]
    barrier = pltpu.get_barrier_semaphore()
    for dy in range(1, ntp):
        pl.semaphore_signal(barrier, inc=1, device_id=tp_at(dy), device_id_type=MESH)
    for dc, dx, dz in others:
        pl.semaphore_signal(barrier, inc=1, device_id=at(dc, dx, dz), device_id_type=MESH)
    loads = []
    for i, (src, dst) in enumerate(
        ((dg_hbm, dg), (du_hbm, du), (dd_hbm, dd), (eg_hbm.at[0], eg), (eu_hbm.at[0], eu), (ed_hbm.at[0], ed))
    ):
        loads.append(pltpu.make_async_copy(src, dst, load_sem.at[i]))
        loads[-1].start()
    scale = scale_ref[...].astype(F32)
    route_weight = scale / jnp.sum(scale, axis=1, keepdims=True)
    lanes = lax.broadcasted_iota(jnp.int32, (rows, own_w.shape[1]), 1)
    table = jnp.zeros((rows, own_w.shape[1]), F32)
    for k in range(routes_ref.shape[1]):
        table = table + jnp.where(lanes == routes_ref[:, k : k + 1], route_weight[:, k : k + 1], 0.0)
    own_w[...] = padded(table, pad_rows)
    weights[0, 0, 0] = own_w[...]
    pl.semaphore_wait(barrier, len(others) + ntp - 1)

    for dy in range(1, ntp):
        send(remote(part_ref, mixed.at[dy - 1], mix_s.at[dy - 1], mix_r.at[dy - 1], tp_at(dy)))
    for dc, dx, dz in others:
        send(
            remote(own_w, weights.at[dc, dx, dz], w_s.at[dc, dx, dz], w_r.at[dc, dx, dz], at(dc, dx, dz))
        )
    total = part_ref[...].astype(F32)
    for dy in range(1, ntp):
        remote(part_ref, mixed.at[dy - 1], mix_s.at[dy - 1], mix_r.at[dy - 1], tp_at(dy)).wait_recv()
        total = total + mixed[dy - 1].astype(F32)
    residual = padded(tokens_ref[...].astype(F32), pad_rows) + total.astype(BF16).astype(F32)
    ffn_f32 = rms_scaled(residual, gain_ref[...])
    ffn_in = ffn_f32.astype(BF16)
    blocks[0, 0, 0] = ffn_in
    for j in range(ntp):
        residual_buf[j] = residual[:, j * cw : (j + 1) * cw]

    def gz(dz):
        return remote(blocks.at[0, 0, 0], blocks.at[0, 0, dz], gz_s.at[dz], gz_r.at[dz], at(0, 0, dz))

    def gx(dx, dz):
        return remote(
            blocks.at[0, 0, dz], blocks.at[0, dx, dz], gx_s.at[dx, dz], gx_r.at[dx, dz], at(0, dx, 0)
        )

    def gc(dc, dx, dz):
        return remote(
            blocks.at[0, dx, dz],
            blocks.at[dc, dx, dz],
            gc_s.at[dc, dx, dz],
            gc_r.at[dc, dx, dz],
            at(dc, 0, 0),
        )

    for dz in range(1, nz):
        send(gz(dz))
    for dx in range(1, nx):
        send(gx(dx, 0))
    for dc in range(1, nc):
        send(gc(dc, 0, 0))

    for load in loads[:3]:
        load.wait()
    dense_hidden = (jax.nn.silu(dot(ffn_in, dg[...])) * dot(ffn_in, du[...])).astype(BF16)
    branch = jax.nn.sigmoid(
        jnp.sum(ffn_in.astype(F32) * wb_ref[...].astype(F32), axis=1, keepdims=True)
    )
    dense = dot(dense_hidden, dd[...]) * branch
    for j in range(ntp):
        acc_buf[j] = dense[:, j * cw : (j + 1) * cw]

    for dz in range(1, nz):
        gz(dz).wait_recv()
        for dx in range(1, nx):
            send(gx(dx, dz))
        for dc in range(1, nc):
            send(gc(dc, 0, dz))
    for dz in range(nz):
        for dx in range(1, nx):
            gx(dx, dz).wait_recv()
            for dc in range(1, nc):
                send(gc(dc, dx, dz))
    for load in loads[3:]:
        load.wait()
    for dc, dx, dz in others:
        remote(
            own_w, weights.at[dc, dx, dz], w_s.at[dc, dx, dz], w_r.at[dc, dx, dz], at(dc, dx, dz)
        ).wait_recv()

    def rc(dc, dx, dz):
        return remote(
            outs.at[dc, dx, dz],
            from_core.at[dc - 1, dx, dz],
            rc_s.at[dc, dx, dz],
            rc_r.at[dc, dx, dz],
            at(-dc, 0, 0),
        )

    def rx(dx, dz):
        return remote(
            summed.at[dx - 1, dz], from_x.at[dx - 1, dz], rx_s.at[dx, dz], rx_r.at[dx, dz], at(0, -dx, 0)
        )

    def rz(dz):
        return remote(to_z.at[dz - 1], from_z.at[dz - 1], rz_s.at[dz], rz_r.at[dz], at(0, 0, -dz))

    count = nx * nz * pad_rows
    for dc in range(nc):
        if dc > 0:
            for dz in range(nz):
                for dx in range(nx):
                    gc(dc, dx, dz).wait_recv()
        inputs = blocks[dc].reshape(count, width)
        gate = jnp.minimum(dot(inputs, eg[...]), CLAMP_LIMIT)
        up = jnp.clip(dot(inputs, eu[...]), -CLAMP_LIMIT, CLAMP_LIMIT)
        hidden = (gate * jax.nn.sigmoid(SWISH_ALPHA * gate) * (up + 1.0)).astype(BF16)
        factor = column(weights[dc].reshape(count, own_w.shape[1]), ep)
        outs[dc] = (dot(hidden, ed[...]) * factor).astype(BF16).reshape(nx, nz, pad_rows, width)
        if dc > 0:
            for dx in list(range(1, nx)) + [0]:
                for dz in list(range(1, nz)) + [0]:
                    send(rc(dc, dx, dz))

    def core_sum(dx, dz):
        value = outs[0, dx, dz].astype(F32)
        for dc in range(1, nc):
            rc(dc, dx, dz).wait_recv()
            value = value + from_core[dc - 1, dx, dz].astype(F32)
        return value

    for dx in range(1, nx):
        for dz in list(range(1, nz)) + [0]:
            summed[dx - 1, dz] = core_sum(dx, dz).astype(BF16)
            send(rx(dx, dz))
    own = None
    for dz in list(range(1, nz)) + [0]:
        value = core_sum(0, dz)
        for dx in range(1, nx):
            rx(dx, dz).wait_recv()
            value = value + from_x[dx - 1, dz].astype(F32)
        if dz > 0:
            to_z[dz - 1] = value.astype(BF16)
            send(rz(dz))
        else:
            own = value
    for dz in range(1, nz):
        rz(dz).wait_recv()
        own = own + from_z[dz - 1].astype(F32)
    for j in range(ntp):
        both = acc_buf[j] + own[:, j * cw : (j + 1) * cw]
        acc_buf[j] = both
        acc_send[j] = both.astype(BF16)

    def ry(dy):
        target = tp_at(dy)
        return remote(acc_send.at[target["tp"]], from_y.at[dy - 1], ry_s.at[dy - 1], ry_r.at[dy - 1], target)

    for dy in range(1, ntp):
        send(ry(dy))
    result = residual_buf[tp] + acc_buf[tp]
    for dy in range(1, ntp):
        ry(dy).wait_recv()
        result = result + from_y[dy - 1].astype(F32)
    out_ref[...] = result[:rows].astype(BF16)
    for copy in pending:
        copy.wait_send()


def local(
    sizes,
    tokens,
    norm_gain,
    w_query,
    w_key,
    w_value,
    w_input_gate,
    w_forget_gate,
    input_bias,
    forget_bias,
    state_c,
    state_n,
    state_m,
    w_mixer_out,
    ffn_gain,
    routes,
    route_scale,
    w_expert_gate,
    w_expert_up,
    w_expert_down,
    w_dense_gate,
    w_dense_up,
    w_dense_down,
    w_branch_gate,
):
    nz, nx, nc, ntp = sizes
    rows, width = tokens.shape
    heads = state_m.shape[1]
    value_size = state_c.shape[3]
    pad_rows = -(-rows // 16) * 16
    cw = width // ntp
    lanes = -(-(nz * nx * nc) // 128) * 128
    vmem = pl.BlockSpec(memory_space=pltpu.VMEM)
    hbm = pl.BlockSpec(memory_space=pl.ANY)
    dma = pltpu.SemaphoreType.DMA
    part, new_c, new_n, new_m = pl.pallas_call(
        cell_kernel,
        name="cell",
        out_shape=(
            jax.ShapeDtypeStruct((pad_rows, width), BF16),
            jax.ShapeDtypeStruct(state_c.shape, F32),
            jax.ShapeDtypeStruct(state_n.shape, F32),
            jax.ShapeDtypeStruct(state_m.shape, F32),
        ),
        in_specs=[vmem] * 9 + [hbm, vmem, vmem, hbm],
        out_specs=(vmem, hbm, vmem, vmem),
        scratch_shapes=[
            pltpu.VMEM(state_c.shape, F32),
            pltpu.VMEM(state_c.shape, F32),
            pltpu.VMEM(w_mixer_out.shape, BF16),
            pltpu.VMEM((pad_rows, heads * value_size), F32),
            dma((rows,)),
            dma((rows,)),
            dma,
        ],
        compiler_params=pltpu.CompilerParams(vmem_limit_bytes=VMEM_LIMIT),
    )(
        tokens,
        norm_gain.reshape(1, width),
        w_query,
        w_key,
        w_value,
        w_input_gate.T,
        w_forget_gate.T,
        input_bias.reshape(1, -1),
        forget_bias.reshape(1, -1),
        state_c,
        state_n,
        state_m,
        w_mixer_out,
    )
    block = (pad_rows, width)
    output = pl.pallas_call(
        functools.partial(ffn_kernel, sizes),
        name="ffn",
        out_shape=jax.ShapeDtypeStruct((rows, cw), BF16),
        in_specs=[vmem] * 6 + [hbm] * 6,
        out_specs=vmem,
        scratch_shapes=[
            pltpu.VMEM(w_expert_gate.shape[1:], BF16),
            pltpu.VMEM(w_expert_up.shape[1:], BF16),
            pltpu.VMEM(w_expert_down.shape[1:], BF16),
            pltpu.VMEM(w_dense_gate.shape, BF16),
            pltpu.VMEM(w_dense_up.shape, BF16),
            pltpu.VMEM(w_dense_down.shape, BF16),
            pltpu.VMEM((max(1, ntp - 1),) + block, BF16),
            pltpu.VMEM((pad_rows, lanes), F32),
            pltpu.VMEM((nc, nx, nz) + block, BF16),
            pltpu.VMEM((nc, nx, nz, pad_rows, lanes), F32),
            pltpu.VMEM((nc, nx, nz) + block, BF16),
            pltpu.VMEM((max(1, nc - 1), nx, nz) + block, BF16),
            pltpu.VMEM((max(1, nx - 1), nz) + block, BF16),
            pltpu.VMEM((max(1, nx - 1), nz) + block, BF16),
            pltpu.VMEM((max(1, nz - 1),) + block, BF16),
            pltpu.VMEM((max(1, nz - 1),) + block, BF16),
            pltpu.VMEM((ntp, pad_rows, cw), F32),
            pltpu.VMEM((ntp, pad_rows, cw), F32),
            pltpu.VMEM((ntp, pad_rows, cw), BF16),
            pltpu.VMEM((max(1, ntp - 1), pad_rows, cw), BF16),
            dma((6,)),
            dma((max(1, ntp - 1),)),
            dma((max(1, ntp - 1),)),
            dma((nc, nx, nz)),
            dma((nc, nx, nz)),
            dma((nz,)),
            dma((nz,)),
            dma((nx, nz)),
            dma((nx, nz)),
            dma((nc, nx, nz)),
            dma((nc, nx, nz)),
            dma((nc, nx, nz)),
            dma((nc, nx, nz)),
            dma((nx, nz)),
            dma((nx, nz)),
            dma((nz,)),
            dma((nz,)),
            dma((max(1, ntp - 1),)),
            dma((max(1, ntp - 1),)),
        ],
        compiler_params=pltpu.CompilerParams(
            vmem_limit_bytes=VMEM_LIMIT, collective_id=0, has_side_effects=True
        ),
    )(
        tokens,
        part,
        ffn_gain.reshape(1, width),
        routes,
        route_scale,
        w_branch_gate.reshape(1, width),
        w_expert_gate,
        w_expert_up,
        w_expert_down,
        w_dense_gate,
        w_dense_up,
        w_dense_down,
    )
    return (output, new_c, new_n, new_m)


def solution(mesh):
    n_ep, n_tp = mesh.shape["ep"], mesh.shape["tp"]
    n_core = 2 if n_ep % 2 == 0 else 1
    n_x = n_tp if n_ep % (n_core * n_tp) == 0 else 1
    sizes = (n_ep // (n_core * n_x), n_x, n_core, n_tp)
    in_specs = (
        P("ep", None),
        P(),
        P(None, "tp"),
        P(None, "tp"),
        P(None, "tp"),
        P(),
        P(),
        P(),
        P(),
        P("ep", "tp", None, None),
        P("ep", "tp", None),
        P("ep", "tp"),
        P("tp", None),
        P(),
        P("ep", None),
        P("ep", None),
        P("ep", None, "tp"),
        P("ep", None, "tp"),
        P("ep", "tp", None),
        P(None, "tp"),
        P(None, "tp"),
        P("tp", None),
        P(),
    )
    out_specs = (P("ep", "tp"), P("ep", "tp", None, None), P("ep", "tp", None), P("ep", "tp"))
    return jax.shard_map(
        functools.partial(local, sizes),
        mesh=mesh,
        in_specs=in_specs,
        out_specs=out_specs,
        check_vma=False,
    )
```

```python
import functools

import jax
import jax.numpy as jnp
from jax import lax
from jax.experimental import pallas as pl
from jax.experimental.pallas import tpu as pltpu
from jax.sharding import PartitionSpec as P

EPSILON = 1e-06
CLAMP_LIMIT = 7.0
SWISH_ALPHA = 1.702
MESH = pl.DeviceIdType.MESH
F32 = jnp.float32
BF16 = jnp.bfloat16
VMEM_LIMIT = 60000 * 1024


def padded(values, rows):
    extra = rows - values.shape[0]
    if extra == 0:
        return values
    return jnp.concatenate([values, jnp.zeros((extra, values.shape[1]), values.dtype)], axis=0)


def dot(left, right):
    return jnp.dot(left, right, preferred_element_type=F32)


def dot_nt(left, right):
    return lax.dot_general(left, right, (((1,), (1,)), ((), ())), preferred_element_type=F32)


def rms_scaled(values, gain):
    scale = lax.rsqrt(jnp.mean(values * values, axis=-1, keepdims=True) + EPSILON)
    return values * scale * gain


def to_column(row, rows):
    shape = (rows, row.shape[1])
    same = lax.broadcasted_iota(jnp.int32, shape, 0) == lax.broadcasted_iota(jnp.int32, shape, 1)
    return jnp.sum(jnp.where(same, row, 0.0), axis=1, keepdims=True)


def to_row(col, lanes):
    shape = (col.shape[0], lanes)
    same = lax.broadcasted_iota(jnp.int32, shape, 0) == lax.broadcasted_iota(jnp.int32, shape, 1)
    return jnp.sum(jnp.where(same, col, 0.0), axis=0, keepdims=True)


def column(values, index):
    lanes = lax.broadcasted_iota(jnp.int32, values.shape, 1)
    return jnp.sum(jnp.where(lanes == index, values, 0.0), axis=1, keepdims=True)


def cell_kernel(
    tokens_hbm,
    gain_hbm,
    wi_hbm,
    wf_hbm,
    ib_hbm,
    fb_hbm,
    m_hbm,
    n_hbm,
    wq_hbm,
    wk_hbm,
    wv_hbm,
    c_hbm,
    mix_hbm,
    part_ref,
    newc_hbm,
    newn_ref,
    newm_ref,
    tokens_ref,
    gain_ref,
    wi_ref,
    wf_ref,
    ib_ref,
    fb_ref,
    m_ref,
    n_ref,
    wq_ref,
    wk_ref,
    wv_ref,
    c_buf,
    co_buf,
    mix_buf,
    num_buf,
    load_sem,
    in_sem,
    out_sem,
    mix_sem,
):
    loads = []
    for i, (src, dst) in enumerate(
        (
            (tokens_hbm, tokens_ref),
            (gain_hbm, gain_ref),
            (wi_hbm, wi_ref),
            (wf_hbm, wf_ref),
            (ib_hbm, ib_ref),
            (fb_hbm, fb_ref),
            (m_hbm, m_ref),
            (n_hbm, n_ref),
            (wq_hbm, wq_ref),
            (wk_hbm, wk_ref),
            (wv_hbm, wv_ref),
        )
    ):
        loads.append(pltpu.make_async_copy(src, dst, load_sem.at[i]))
        loads[-1].start()
    rows = tokens_ref.shape[0]
    pad_rows = part_ref.shape[0]
    heads = m_ref.shape[0]
    dk, dv = c_buf.shape[2], c_buf.shape[3]
    first = lax.axis_index("tp") * heads
    for t in range(rows):
        pltpu.make_async_copy(c_hbm.at[t], c_buf.at[t], in_sem.at[t]).start()
    pltpu.make_async_copy(mix_hbm, mix_buf, mix_sem).start()
    for load in loads[:8]:
        load.wait()
    tokens = padded(tokens_ref[...].astype(F32), pad_rows)
    normed = rms_scaled(tokens, gain_ref[...]).astype(BF16)
    for load in loads[8:]:
        load.wait()
    queries = dot(normed, wq_ref[...]).astype(BF16).astype(F32)
    keys = dot(normed, wk_ref[...]).astype(BF16).astype(F32)
    values = dot(normed, wv_ref[...]).astype(BF16).astype(F32)
    pre_all = dot_nt(normed, wi_ref[...]) + ib_ref[...]
    fg_all = dot_nt(normed, wf_ref[...]) + fb_ref[...]
    fg_all = jnp.minimum(fg_all, 0.0) - jnp.log(1.0 + jnp.exp(-jnp.abs(fg_all)))
    key_scale = dk**-0.5
    per_head = []
    for h in range(heads):
        pre = column(pre_all, first + h)
        shifted = column(fg_all, first + h) + to_column(m_ref[h : h + 1, :], pad_rows)
        new_m = jnp.maximum(shifted, pre)
        forget = jnp.exp(shifted - new_m)
        inflow = jnp.exp(pre - new_m)
        newm_ref[h : h + 1, :] = to_row(new_m, rows)
        q = queries[:, h * dk : (h + 1) * dk]
        k = keys[:, h * dk : (h + 1) * dk] * (inflow * key_scale)
        v = values[:, h * dv : (h + 1) * dv]
        new_n = forget * padded(n_ref[:, h, :], pad_rows) + k
        newn_ref[:, h, :] = new_n[:rows]
        denom = jnp.maximum(jnp.abs(jnp.sum(q * new_n, axis=1, keepdims=True)), 1.0)
        per_head.append((forget, q.T, k.T, v, denom))
    num_buf[...] = jnp.zeros(num_buf.shape, F32)
    for t in range(rows):
        pltpu.make_async_copy(c_hbm.at[t], c_buf.at[t], in_sem.at[t]).wait()
        for h in range(heads):
            forget, q_t, k_t, v, _ = per_head[h]
            new_c = forget[t : t + 1] * c_buf[t, h] + k_t[:, t : t + 1] * v[t : t + 1]
            co_buf[t, h] = new_c
            num_buf[t : t + 1, h * dv : (h + 1) * dv] = jnp.sum(
                q_t[:, t : t + 1] * new_c, axis=0, keepdims=True
            )
        pltpu.make_async_copy(co_buf.at[t], newc_hbm.at[t], out_sem.at[t]).start()
    head_out = jnp.concatenate(
        [num_buf[:, h * dv : (h + 1) * dv] / per_head[h][4] for h in range(heads)], axis=1
    ).astype(BF16)
    pltpu.make_async_copy(mix_hbm, mix_buf, mix_sem).wait()
    part_ref[...] = dot(head_out, mix_buf[...]).astype(BF16)
    for t in range(rows):
        pltpu.make_async_copy(co_buf.at[t], newc_hbm.at[t], out_sem.at[t]).wait()


def ffn_kernel(
    sizes,
    tokens_hbm,
    part_hbm,
    gain_hbm,
    routes_hbm,
    scale_hbm,
    wb_hbm,
    eg_hbm,
    eu_hbm,
    ed_hbm,
    dg_hbm,
    du_hbm,
    dd_hbm,
    out_ref,
    tokens_ref,
    part_ref,
    gain_ref,
    routes_ref,
    scale_ref,
    wb_ref,
    eg,
    eu,
    ed,
    dg,
    du,
    dd,
    mixed,
    own_w,
    blocks,
    weights,
    outs,
    from_core,
    summed,
    from_x,
    to_z,
    from_z,
    residual_buf,
    acc_buf,
    acc_send,
    from_y,
    load_sem,
    mix_s,
    mix_r,
    w_s,
    w_r,
    gz_s,
    gz_r,
    gx_s,
    gx_r,
    gc_s,
    gc_r,
    rc_s,
    rc_r,
    rx_s,
    rx_r,
    rz_s,
    rz_r,
    ry_s,
    ry_r,
):
    nz, nx, nc, ntp = sizes
    ep = lax.axis_index("ep")
    tp = lax.axis_index("tp")
    c = lax.rem(ep, nc)
    x = lax.rem(lax.div(ep, nc), nx)
    z = lax.div(ep, nc * nx)
    rows, width = tokens_ref.shape
    pad_rows = part_ref.shape[0]
    cw = width // ntp

    def at(dc, dx, dz):
        return {
            "ep": (lax.rem(z + dz + nz, nz) * nx + lax.rem(x + dx + nx, nx)) * nc
            + lax.rem(c + dc + nc, nc)
        }

    def tp_at(dy):
        return {"tp": lax.rem(tp + dy + ntp, ntp)}

    def remote(src, dst, send, recv, device):
        return pltpu.make_async_remote_copy(
            src_ref=src, dst_ref=dst, send_sem=send, recv_sem=recv, device_id=device, device_id_type=MESH
        )

    pending = []

    def send(copy):
        copy.start()
        pending.append(copy)

    others = [
        (dc, dx, dz)
        for dc in range(nc)
        for dx in range(nx)
        for dz in range(nz)
        if (dc, dx, dz) != (0, 0, 0)
    ]
    barrier = pltpu.get_barrier_semaphore()
    for dy in range(1, ntp):
        pl.semaphore_signal(barrier, inc=1, device_id=tp_at(dy), device_id_type=MESH)
    for dc, dx, dz in others:
        pl.semaphore_signal(barrier, inc=1, device_id=at(dc, dx, dz), device_id_type=MESH)
    loads = []
    for i, (src, dst) in enumerate(
        (
            (routes_hbm, routes_ref),
            (scale_hbm, scale_ref),
            (tokens_hbm, tokens_ref),
            (part_hbm, part_ref),
            (gain_hbm, gain_ref),
            (wb_hbm, wb_ref),
            (dg_hbm, dg),
            (du_hbm, du),
            (dd_hbm, dd),
            (eg_hbm.at[0], eg),
            (eu_hbm.at[0], eu),
            (ed_hbm.at[0], ed),
        )
    ):
        loads.append(pltpu.make_async_copy(src, dst, load_sem.at[i]))
        loads[-1].start()
    for load in loads[:2]:
        load.wait()
    scale = scale_ref[...].astype(F32)
    route_weight = scale / jnp.sum(scale, axis=0, keepdims=True)
    experts = own_w.shape[0]
    ids = lax.broadcasted_iota(jnp.int32, (experts, rows), 0)
    table = jnp.zeros((experts, rows), F32)
    for k in range(routes_ref.shape[0]):
        table = table + jnp.where(ids == routes_ref[k : k + 1, :], route_weight[k : k + 1, :], 0.0)
    table = jnp.concatenate([table, jnp.zeros((experts, own_w.shape[2] - rows), F32)], axis=1)
    for e in range(experts):
        own_w[e] = table[e : e + 1, :]
    for load in loads[2:6]:
        load.wait()
    pl.semaphore_wait(barrier, len(others) + ntp - 1)

    def wt(dc, dx, dz):
        target = at(dc, dx, dz)
        return remote(
            own_w.at[target["ep"]], weights.at[dc, dx, dz], w_s.at[dc, dx, dz], w_r.at[dc, dx, dz], target
        )

    for dy in range(1, ntp):
        send(remote(part_ref, mixed.at[dy - 1], mix_s.at[dy - 1], mix_r.at[dy - 1], tp_at(dy)))
    for dc, dx, dz in others:
        send(wt(dc, dx, dz))
    weights[0, 0, 0] = own_w[ep]
    total = part_ref[...].astype(F32)
    for dy in range(1, ntp):
        remote(part_ref, mixed.at[dy - 1], mix_s.at[dy - 1], mix_r.at[dy - 1], tp_at(dy)).wait_recv()
        total = total + mixed[dy - 1].astype(F32)
    residual = padded(tokens_ref[...].astype(F32), pad_rows) + total.astype(BF16).astype(F32)
    ffn_f32 = rms_scaled(residual, gain_ref[...])
    ffn_in = ffn_f32.astype(BF16)
    blocks[0, 0, 0] = ffn_in
    for j in range(ntp):
        residual_buf[j] = residual[:, j * cw : (j + 1) * cw]

    def gz(dz):
        return remote(blocks.at[0, 0, 0], blocks.at[0, 0, dz], gz_s.at[dz], gz_r.at[dz], at(0, 0, dz))

    def gx(dx, dz):
        return remote(
            blocks.at[0, 0, dz], blocks.at[0, dx, dz], gx_s.at[dx, dz], gx_r.at[dx, dz], at(0, dx, 0)
        )

    def gc(dc, dx, dz):
        return remote(
            blocks.at[0, dx, dz],
            blocks.at[dc, dx, dz],
            gc_s.at[dc, dx, dz],
            gc_r.at[dc, dx, dz],
            at(dc, 0, 0),
        )

    for dz in range(1, nz):
        send(gz(dz))
    for dx in range(1, nx):
        send(gx(dx, 0))
    for dc in range(1, nc):
        send(gc(dc, 0, 0))

    for load in loads[6:9]:
        load.wait()
    dense_hidden = (jax.nn.silu(dot(ffn_in, dg[...])) * dot(ffn_in, du[...])).astype(BF16)
    wb = wb_ref[...].astype(F32)
    lanes = wb.shape[1]
    wide = ffn_in.astype(F32)
    branch = jnp.zeros((pad_rows, lanes), F32)
    for i in range(wb.shape[0]):
        branch = branch + wide[:, i * lanes : (i + 1) * lanes] * wb[i : i + 1, :]
    branch = jax.nn.sigmoid(jnp.sum(branch, axis=1, keepdims=True))
    dense = dot(dense_hidden, dd[...]) * branch
    for j in range(ntp):
        acc_buf[j] = dense[:, j * cw : (j + 1) * cw]

    for dz in range(1, nz):
        gz(dz).wait_recv()
        for dx in range(1, nx):
            send(gx(dx, dz))
        for dc in range(1, nc):
            send(gc(dc, 0, dz))
    for dz in range(nz):
        for dx in range(1, nx):
            gx(dx, dz).wait_recv()
            for dc in range(1, nc):
                send(gc(dc, dx, dz))
    for load in loads[9:]:
        load.wait()
    for dc, dx, dz in others:
        wt(dc, dx, dz).wait_recv()

    def rc(dc, dx, dz):
        return remote(
            outs.at[dc, dx, dz],
            from_core.at[dc - 1, dx, dz],
            rc_s.at[dc, dx, dz],
            rc_r.at[dc, dx, dz],
            at(-dc, 0, 0),
        )

    def rx(dx, dz):
        return remote(
            summed.at[dx - 1, dz], from_x.at[dx - 1, dz], rx_s.at[dx, dz], rx_r.at[dx, dz], at(0, -dx, 0)
        )

    def rz(dz):
        return remote(to_z.at[dz - 1], from_z.at[dz - 1], rz_s.at[dz], rz_r.at[dz], at(0, 0, -dz))

    count = nx * nz * pad_rows
    for dc in range(nc):
        if dc > 0:
            for dz in range(nz):
                for dx in range(nx):
                    gc(dc, dx, dz).wait_recv()
        inputs = blocks[dc].reshape(count, width)
        gate = jnp.minimum(dot(inputs, eg[...]), CLAMP_LIMIT)
        up = jnp.clip(dot(inputs, eu[...]), -CLAMP_LIMIT, CLAMP_LIMIT)
        hidden = (gate * jax.nn.sigmoid(SWISH_ALPHA * gate) * (up + 1.0)).astype(BF16)
        factor = jnp.concatenate(
            [to_column(weights[dc, dx, dz], pad_rows) for dx in range(nx) for dz in range(nz)], axis=0
        )
        outs[dc] = (dot(hidden, ed[...]) * factor).astype(BF16).reshape(nx, nz, pad_rows, width)
        if dc > 0:
            for dx in list(range(1, nx)) + [0]:
                for dz in list(range(1, nz)) + [0]:
                    send(rc(dc, dx, dz))

    def core_sum(dx, dz):
        value = outs[0, dx, dz].astype(F32)
        for dc in range(1, nc):
            rc(dc, dx, dz).wait_recv()
            value = value + from_core[dc - 1, dx, dz].astype(F32)
        return value

    for dx in range(1, nx):
        for dz in list(range(1, nz)) + [0]:
            summed[dx - 1, dz] = core_sum(dx, dz).astype(BF16)
            send(rx(dx, dz))
    own = None
    for dz in list(range(1, nz)) + [0]:
        value = core_sum(0, dz)
        for dx in range(1, nx):
            rx(dx, dz).wait_recv()
            value = value + from_x[dx - 1, dz].astype(F32)
        if dz > 0:
            to_z[dz - 1] = value.astype(BF16)
            send(rz(dz))
        else:
            own = value
    for dz in range(1, nz):
        rz(dz).wait_recv()
        own = own + from_z[dz - 1].astype(F32)
    for j in range(ntp):
        both = acc_buf[j] + own[:, j * cw : (j + 1) * cw]
        acc_buf[j] = both
        acc_send[j] = both.astype(BF16)

    def ry(dy):
        target = tp_at(dy)
        return remote(acc_send.at[target["tp"]], from_y.at[dy - 1], ry_s.at[dy - 1], ry_r.at[dy - 1], target)

    for dy in range(1, ntp):
        send(ry(dy))
    result = residual_buf[tp] + acc_buf[tp]
    for dy in range(1, ntp):
        ry(dy).wait_recv()
        result = result + from_y[dy - 1].astype(F32)
    out_ref[...] = result[:rows].astype(BF16)
    for copy in pending:
        copy.wait_send()


def local(
    sizes,
    tokens,
    norm_gain,
    w_query,
    w_key,
    w_value,
    w_input_gate,
    w_forget_gate,
    input_bias,
    forget_bias,
    state_c,
    state_n,
    state_m,
    w_mixer_out,
    ffn_gain,
    routes,
    route_scale,
    w_expert_gate,
    w_expert_up,
    w_expert_down,
    w_dense_gate,
    w_dense_up,
    w_dense_down,
    w_branch_gate,
):
    nz, nx, nc, ntp = sizes
    rows, width = tokens.shape
    heads = state_m.shape[1]
    value_size = state_c.shape[3]
    pad_rows = -(-rows // 16) * 16
    cw = width // ntp
    vmem = pl.BlockSpec(memory_space=pltpu.VMEM)
    hbm = pl.BlockSpec(memory_space=pl.ANY)
    dma = pltpu.SemaphoreType.DMA
    part, new_c, new_n, new_m = pl.pallas_call(
        cell_kernel,
        name="cell",
        out_shape=(
            jax.ShapeDtypeStruct((pad_rows, width), BF16),
            jax.ShapeDtypeStruct(state_c.shape, F32),
            jax.ShapeDtypeStruct(state_n.shape, F32),
            jax.ShapeDtypeStruct(state_m.shape[::-1], F32),
        ),
        in_specs=[hbm] * 13,
        out_specs=(vmem, hbm, vmem, vmem),
        scratch_shapes=[
            pltpu.VMEM(tokens.shape, BF16),
            pltpu.VMEM((1, width), F32),
            pltpu.VMEM(w_input_gate.shape[::-1], BF16),
            pltpu.VMEM(w_forget_gate.shape[::-1], BF16),
            pltpu.VMEM((1, input_bias.shape[0]), F32),
            pltpu.VMEM((1, forget_bias.shape[0]), F32),
            pltpu.VMEM(state_m.shape[::-1], F32),
            pltpu.VMEM(state_n.shape, F32),
            pltpu.VMEM(w_query.shape, BF16),
            pltpu.VMEM(w_key.shape, BF16),
            pltpu.VMEM(w_value.shape, BF16),
            pltpu.VMEM(state_c.shape, F32),
            pltpu.VMEM(state_c.shape, F32),
            pltpu.VMEM(w_mixer_out.shape, BF16),
            pltpu.VMEM((pad_rows, heads * value_size), F32),
            dma((11,)),
            dma((rows,)),
            dma((rows,)),
            dma,
        ],
        compiler_params=pltpu.CompilerParams(vmem_limit_bytes=VMEM_LIMIT),
    )(
        tokens,
        norm_gain.reshape(1, width),
        w_input_gate.T,
        w_forget_gate.T,
        input_bias.reshape(1, -1),
        forget_bias.reshape(1, -1),
        state_m.T,
        state_n,
        w_query,
        w_key,
        w_value,
        state_c,
        w_mixer_out,
    )
    block = (pad_rows, width)
    output = pl.pallas_call(
        functools.partial(ffn_kernel, sizes),
        name="ffn",
        out_shape=jax.ShapeDtypeStruct((rows, cw), BF16),
        in_specs=[hbm] * 12,
        out_specs=vmem,
        scratch_shapes=[
            pltpu.VMEM(tokens.shape, BF16),
            pltpu.VMEM(block, BF16),
            pltpu.VMEM((1, width), F32),
            pltpu.VMEM(routes.shape[::-1], jnp.int32),
            pltpu.VMEM(route_scale.shape[::-1], BF16),
            pltpu.VMEM((width // 128, 128), BF16),
            pltpu.VMEM(w_expert_gate.shape[1:], BF16),
            pltpu.VMEM(w_expert_up.shape[1:], BF16),
            pltpu.VMEM(w_expert_down.shape[1:], BF16),
            pltpu.VMEM(w_dense_gate.shape, BF16),
            pltpu.VMEM(w_dense_up.shape, BF16),
            pltpu.VMEM(w_dense_down.shape, BF16),
            pltpu.VMEM((max(1, ntp - 1),) + block, BF16),
            pltpu.VMEM((nz * nx * nc, 1, 128), F32),
            pltpu.VMEM((nc, nx, nz) + block, BF16),
            pltpu.VMEM((nc, nx, nz, 1, 128), F32),
            pltpu.VMEM((nc, nx, nz) + block, BF16),
            pltpu.VMEM((max(1, nc - 1), nx, nz) + block, BF16),
            pltpu.VMEM((max(1, nx - 1), nz) + block, BF16),
            pltpu.VMEM((max(1, nx - 1), nz) + block, BF16),
            pltpu.VMEM((max(1, nz - 1),) + block, BF16),
            pltpu.VMEM((max(1, nz - 1),) + block, BF16),
            pltpu.VMEM((ntp, pad_rows, cw), F32),
            pltpu.VMEM((ntp, pad_rows, cw), F32),
            pltpu.VMEM((ntp, pad_rows, cw), BF16),
            pltpu.VMEM((max(1, ntp - 1), pad_rows, cw), BF16),
            dma((12,)),
            dma((max(1, ntp - 1),)),
            dma((max(1, ntp - 1),)),
            dma((nc, nx, nz)),
            dma((nc, nx, nz)),
            dma((nz,)),
            dma((nz,)),
            dma((nx, nz)),
            dma((nx, nz)),
            dma((nc, nx, nz)),
            dma((nc, nx, nz)),
            dma((nc, nx, nz)),
            dma((nc, nx, nz)),
            dma((nx, nz)),
            dma((nx, nz)),
            dma((nz,)),
            dma((nz,)),
            dma((max(1, ntp - 1),)),
            dma((max(1, ntp - 1),)),
        ],
        compiler_params=pltpu.CompilerParams(
            vmem_limit_bytes=VMEM_LIMIT, collective_id=0, has_side_effects=True
        ),
    )(
        tokens,
        part,
        ffn_gain.reshape(1, width),
        routes.T,
        route_scale.T,
        w_branch_gate.reshape(width // 128, 128),
        w_expert_gate,
        w_expert_up,
        w_expert_down,
        w_dense_gate,
        w_dense_up,
        w_dense_down,
    )
    return (output, new_c, new_n, new_m.T)


def solution(mesh):
    n_ep, n_tp = mesh.shape["ep"], mesh.shape["tp"]
    n_core = 2 if n_ep % 2 == 0 else 1
    n_x = n_tp if n_ep % (n_core * n_tp) == 0 else 1
    sizes = (n_ep // (n_core * n_x), n_x, n_core, n_tp)
    in_specs = (
        P("ep", None),
        P(),
        P(None, "tp"),
        P(None, "tp"),
        P(None, "tp"),
        P(),
        P(),
        P(),
        P(),
        P("ep", "tp", None, None),
        P("ep", "tp", None),
        P("ep", "tp"),
        P("tp", None),
        P(),
        P("ep", None),
        P("ep", None),
        P("ep", None, "tp"),
        P("ep", None, "tp"),
        P("ep", "tp", None),
        P(None, "tp"),
        P(None, "tp"),
        P("tp", None),
        P(),
    )
    out_specs = (P("ep", "tp"), P("ep", "tp", None, None), P("ep", "tp", None), P("ep", "tp"))
    return jax.shard_map(
        functools.partial(local, sizes),
        mesh=mesh,
        in_specs=in_specs,
        out_specs=out_specs,
        check_vma=False,
    )
```

```python
import functools

import jax
import jax.numpy as jnp
from jax import lax
from jax.experimental import pallas as pl
from jax.experimental.pallas import tpu as pltpu
from jax.sharding import PartitionSpec as P

EPSILON = 1e-06
CLAMP_LIMIT = 7.0
SWISH_ALPHA = 1.702
MESH = pl.DeviceIdType.MESH
F32 = jnp.float32
BF16 = jnp.bfloat16
VMEM_LIMIT = 60000 * 1024


def padded(values, rows):
    extra = rows - values.shape[0]
    if extra == 0:
        return values
    return jnp.concatenate([values, jnp.zeros((extra, values.shape[1]), values.dtype)], axis=0)


def dot(left, right):
    return jnp.dot(left, right, preferred_element_type=F32)


def dot_nt(left, right):
    return lax.dot_general(left, right, (((1,), (1,)), ((), ())), preferred_element_type=F32)


def rms_scaled(values, gain):
    scale = lax.rsqrt(jnp.mean(values * values, axis=-1, keepdims=True) + EPSILON)
    return values * scale * gain


def to_column(row, rows):
    shape = (rows, row.shape[1])
    same = lax.broadcasted_iota(jnp.int32, shape, 0) == lax.broadcasted_iota(jnp.int32, shape, 1)
    return jnp.sum(jnp.where(same, row, 0.0), axis=1, keepdims=True)


def to_row(col, lanes):
    shape = (col.shape[0], lanes)
    same = lax.broadcasted_iota(jnp.int32, shape, 0) == lax.broadcasted_iota(jnp.int32, shape, 1)
    return jnp.sum(jnp.where(same, col, 0.0), axis=0, keepdims=True)


def column(values, index):
    lanes = lax.broadcasted_iota(jnp.int32, values.shape, 1)
    return jnp.sum(jnp.where(lanes == index, values, 0.0), axis=1, keepdims=True)


def cell_kernel(
    tokens_hbm,
    gain_hbm,
    wi_hbm,
    wf_hbm,
    ib_hbm,
    fb_hbm,
    m_hbm,
    n_hbm,
    wq_hbm,
    wk_hbm,
    wv_hbm,
    c_hbm,
    mix_hbm,
    part_ref,
    newc_hbm,
    newn_ref,
    newm_ref,
    tokens_ref,
    gain_ref,
    wi_ref,
    wf_ref,
    ib_ref,
    fb_ref,
    m_ref,
    n_ref,
    wq_ref,
    wk_ref,
    wv_ref,
    c_buf,
    co_buf,
    mix_buf,
    num_buf,
    load_sem,
    in_sem,
    out_sem,
    mix_sem,
):
    loads = []
    for i, (src, dst) in enumerate(
        (
            (tokens_hbm, tokens_ref),
            (gain_hbm, gain_ref),
            (wi_hbm, wi_ref),
            (wf_hbm, wf_ref),
            (ib_hbm, ib_ref),
            (fb_hbm, fb_ref),
            (m_hbm, m_ref),
            (n_hbm, n_ref),
            (wq_hbm, wq_ref),
            (wk_hbm, wk_ref),
            (wv_hbm, wv_ref),
        )
    ):
        loads.append(pltpu.make_async_copy(src, dst, load_sem.at[i]))
        loads[-1].start()
    rows = tokens_ref.shape[0]
    pad_rows = part_ref.shape[0]
    heads = m_ref.shape[0]
    dk, dv = c_buf.shape[2], c_buf.shape[3]
    first = lax.axis_index("tp") * heads
    for t in range(rows):
        pltpu.make_async_copy(c_hbm.at[t], c_buf.at[t], in_sem.at[t]).start()
    pltpu.make_async_copy(mix_hbm, mix_buf, mix_sem).start()
    for load in loads[:8]:
        load.wait()
    tokens = padded(tokens_ref[...].astype(F32), pad_rows)
    normed = rms_scaled(tokens, gain_ref[...]).astype(BF16)
    for load in loads[8:]:
        load.wait()
    queries = dot(normed, wq_ref[...]).astype(BF16).astype(F32)
    keys = dot(normed, wk_ref[...]).astype(BF16).astype(F32)
    values = dot(normed, wv_ref[...]).astype(BF16).astype(F32)
    pre_all = dot_nt(normed, wi_ref[...]) + ib_ref[...]
    fg_all = dot_nt(normed, wf_ref[...]) + fb_ref[...]
    fg_all = jnp.minimum(fg_all, 0.0) - jnp.log(1.0 + jnp.exp(-jnp.abs(fg_all)))
    key_scale = dk**-0.5
    per_head = []
    for h in range(heads):
        pre = column(pre_all, first + h)
        shifted = column(fg_all, first + h) + to_column(m_ref[h : h + 1, :], pad_rows)
        new_m = jnp.maximum(shifted, pre)
        forget = jnp.exp(shifted - new_m)
        inflow = jnp.exp(pre - new_m)
        newm_ref[h : h + 1, :] = to_row(new_m, rows)
        q = queries[:, h * dk : (h + 1) * dk]
        k = keys[:, h * dk : (h + 1) * dk] * (inflow * key_scale)
        v = values[:, h * dv : (h + 1) * dv]
        new_n = forget * padded(n_ref[:, h, :], pad_rows) + k
        newn_ref[:, h, :] = new_n[:rows]
        denom = jnp.maximum(jnp.abs(jnp.sum(q * new_n, axis=1, keepdims=True)), 1.0)
        per_head.append((forget, q.T, k.T, v, denom))
    num_buf[...] = jnp.zeros(num_buf.shape, F32)
    for t in range(rows):
        pltpu.make_async_copy(c_hbm.at[t], c_buf.at[t], in_sem.at[t]).wait()
        for h in range(heads):
            forget, q_t, k_t, v, _ = per_head[h]
            new_c = forget[t : t + 1] * c_buf[t, h] + k_t[:, t : t + 1] * v[t : t + 1]
            co_buf[t, h] = new_c
            num_buf[t : t + 1, h * dv : (h + 1) * dv] = jnp.sum(
                q_t[:, t : t + 1] * new_c, axis=0, keepdims=True
            )
        pltpu.make_async_copy(co_buf.at[t], newc_hbm.at[t], out_sem.at[t]).start()
    head_out = jnp.concatenate(
        [num_buf[:, h * dv : (h + 1) * dv] / per_head[h][4] for h in range(heads)], axis=1
    ).astype(BF16)
    pltpu.make_async_copy(mix_hbm, mix_buf, mix_sem).wait()
    part_ref[...] = dot(head_out, mix_buf[...]).astype(BF16)
    for t in range(rows):
        pltpu.make_async_copy(co_buf.at[t], newc_hbm.at[t], out_sem.at[t]).wait()


def ffn_kernel(
    sizes,
    tokens_hbm,
    part_hbm,
    gain_hbm,
    routes_hbm,
    scale_hbm,
    wb_hbm,
    eg_hbm,
    eu_hbm,
    ed_hbm,
    dg_hbm,
    du_hbm,
    dd_hbm,
    out_ref,
    tokens_ref,
    part_ref,
    gain_ref,
    routes_ref,
    scale_ref,
    wb_ref,
    eg,
    eu,
    ed,
    dg,
    du,
    dd,
    mixed,
    own_w,
    blocks,
    weights,
    outs,
    from_core,
    summed,
    from_x,
    to_z,
    from_z,
    residual_buf,
    acc_buf,
    acc_send,
    from_y,
    load_sem,
    mix_s,
    mix_r,
    w_s,
    w_r,
    gz_s,
    gz_r,
    gx_s,
    gx_r,
    gc_s,
    gc_r,
    rc_s,
    rc_r,
    rx_s,
    rx_r,
    rz_s,
    rz_r,
    ry_s,
    ry_r,
):
    nz, nx, nc, ntp = sizes
    ep = lax.axis_index("ep")
    tp = lax.axis_index("tp")
    c = lax.rem(ep, nc)
    x = lax.rem(lax.div(ep, nc), nx)
    z = lax.div(ep, nc * nx)
    rows, width = tokens_ref.shape
    pad_rows = part_ref.shape[0]
    cw = width // ntp

    def at(dc, dx, dz):
        return {
            "ep": (lax.rem(z + dz + nz, nz) * nx + lax.rem(x + dx + nx, nx)) * nc
            + lax.rem(c + dc + nc, nc)
        }

    def tp_at(dy):
        return {"tp": lax.rem(tp + dy + ntp, ntp)}

    def remote(src, dst, send, recv, device):
        return pltpu.make_async_remote_copy(
            src_ref=src, dst_ref=dst, send_sem=send, recv_sem=recv, device_id=device, device_id_type=MESH
        )

    pending = []

    def send(copy):
        copy.start()
        pending.append(copy)

    others = [
        (dc, dx, dz)
        for dc in range(nc)
        for dx in range(nx)
        for dz in range(nz)
        if (dc, dx, dz) != (0, 0, 0)
    ]
    barrier = pltpu.get_barrier_semaphore()
    for dy in range(1, ntp):
        pl.semaphore_signal(barrier, inc=1, device_id=tp_at(dy), device_id_type=MESH)
    for dc, dx, dz in others:
        pl.semaphore_signal(barrier, inc=1, device_id=at(dc, dx, dz), device_id_type=MESH)
    loads = []
    for i, (src, dst) in enumerate(
        (
            (routes_hbm, routes_ref),
            (scale_hbm, scale_ref),
            (tokens_hbm, tokens_ref),
            (part_hbm, part_ref),
            (gain_hbm, gain_ref),
            (wb_hbm, wb_ref),
            (dg_hbm, dg),
            (du_hbm, du),
            (dd_hbm, dd),
            (eg_hbm.at[0], eg),
            (eu_hbm.at[0], eu),
            (ed_hbm.at[0], ed),
        )
    ):
        loads.append(pltpu.make_async_copy(src, dst, load_sem.at[i]))
        loads[-1].start()
    for load in loads[:2]:
        load.wait()
    scale = scale_ref[...].astype(F32)
    route_weight = scale / jnp.sum(scale, axis=0, keepdims=True)
    experts = own_w.shape[0]
    ids = lax.broadcasted_iota(jnp.int32, (experts, rows), 0)
    table = jnp.zeros((experts, rows), F32)
    for k in range(routes_ref.shape[0]):
        table = table + jnp.where(ids == routes_ref[k : k + 1, :], route_weight[k : k + 1, :], 0.0)
    table = jnp.concatenate([table, jnp.zeros((experts, own_w.shape[2] - rows), F32)], axis=1)
    for e in range(experts):
        own_w[e] = table[e : e + 1, :]
    for load in loads[2:6]:
        load.wait()
    pl.semaphore_wait(barrier, len(others) + ntp - 1)

    def wt(dc, dx, dz):
        target = at(dc, dx, dz)
        return remote(
            own_w.at[target["ep"]], weights.at[dc, dx, dz], w_s.at[dc, dx, dz], w_r.at[dc, dx, dz], target
        )

    for dy in range(1, ntp):
        send(remote(part_ref, mixed.at[dy - 1], mix_s.at[dy - 1], mix_r.at[dy - 1], tp_at(dy)))
    for dc, dx, dz in others:
        send(wt(dc, dx, dz))
    weights[0, 0, 0] = own_w[ep]
    total = part_ref[...].astype(F32)
    for dy in range(1, ntp):
        remote(part_ref, mixed.at[dy - 1], mix_s.at[dy - 1], mix_r.at[dy - 1], tp_at(dy)).wait_recv()
        total = total + mixed[dy - 1].astype(F32)
    residual = padded(tokens_ref[...].astype(F32), pad_rows) + total.astype(BF16).astype(F32)
    ffn_f32 = rms_scaled(residual, gain_ref[...])
    ffn_in = ffn_f32.astype(BF16)
    blocks[0, 0, 0] = ffn_in
    for j in range(ntp):
        residual_buf[j] = residual[:, j * cw : (j + 1) * cw]

    def gz(dz):
        return remote(blocks.at[0, 0, 0], blocks.at[0, 0, dz], gz_s.at[dz], gz_r.at[dz], at(0, 0, dz))

    def gx(dx, dz):
        return remote(
            blocks.at[0, 0, dz], blocks.at[0, dx, dz], gx_s.at[dx, dz], gx_r.at[dx, dz], at(0, dx, 0)
        )

    def gc(dc, dx, dz):
        return remote(
            blocks.at[0, dx, dz],
            blocks.at[dc, dx, dz],
            gc_s.at[dc, dx, dz],
            gc_r.at[dc, dx, dz],
            at(dc, 0, 0),
        )

    for dz in range(1, nz):
        send(gz(dz))
    for dx in range(1, nx):
        send(gx(dx, 0))
    for dc in range(1, nc):
        send(gc(dc, 0, 0))

    for load in loads[6:9]:
        load.wait()
    dense_hidden = (jax.nn.silu(dot(ffn_in, dg[...])) * dot(ffn_in, du[...])).astype(BF16)
    wb = wb_ref[...].astype(F32)
    lanes = wb.shape[1]
    wide = ffn_in.astype(F32)
    branch = jnp.zeros((pad_rows, lanes), F32)
    for i in range(wb.shape[0]):
        branch = branch + wide[:, i * lanes : (i + 1) * lanes] * wb[i : i + 1, :]
    branch = jax.nn.sigmoid(jnp.sum(branch, axis=1, keepdims=True))
    dense = dot(dense_hidden, dd[...]) * branch
    for j in range(ntp):
        acc_buf[j] = dense[:, j * cw : (j + 1) * cw]

    for dz in range(1, nz):
        gz(dz).wait_recv()
        for dx in range(1, nx):
            send(gx(dx, dz))
        for dc in range(1, nc):
            send(gc(dc, 0, dz))
    for dz in range(nz):
        for dx in range(1, nx):
            gx(dx, dz).wait_recv()
            for dc in range(1, nc):
                send(gc(dc, dx, dz))
    for load in loads[9:]:
        load.wait()
    for dc, dx, dz in others:
        wt(dc, dx, dz).wait_recv()

    def rc(dc, dx, dz):
        return remote(
            outs.at[dc, dx, dz],
            from_core.at[dc - 1, dx, dz],
            rc_s.at[dc, dx, dz],
            rc_r.at[dc, dx, dz],
            at(-dc, 0, 0),
        )

    def rx(dx, dz):
        return remote(
            summed.at[dx - 1, dz], from_x.at[dx - 1, dz], rx_s.at[dx, dz], rx_r.at[dx, dz], at(0, -dx, 0)
        )

    def rz(dz):
        return remote(to_z.at[dz - 1], from_z.at[dz - 1], rz_s.at[dz], rz_r.at[dz], at(0, 0, -dz))

    count = nx * nz * pad_rows
    for dc in range(nc):
        if dc > 0:
            for dz in range(nz):
                for dx in range(nx):
                    gc(dc, dx, dz).wait_recv()
        inputs = blocks[dc].reshape(count, width)
        gate = jnp.minimum(dot(inputs, eg[...]), CLAMP_LIMIT)
        up = jnp.clip(dot(inputs, eu[...]), -CLAMP_LIMIT, CLAMP_LIMIT)
        hidden = (gate * jax.nn.sigmoid(SWISH_ALPHA * gate) * (up + 1.0)).astype(BF16)
        factor = jnp.concatenate(
            [to_column(weights[dc, dx, dz], pad_rows) for dx in range(nx) for dz in range(nz)], axis=0
        )
        outs[dc] = (dot(hidden, ed[...]) * factor).astype(BF16).reshape(nx, nz, pad_rows, width)
        if dc > 0:
            for dx in list(range(1, nx)) + [0]:
                for dz in list(range(1, nz)) + [0]:
                    send(rc(dc, dx, dz))

    def core_sum(dx, dz):
        value = outs[0, dx, dz].astype(F32)
        for dc in range(1, nc):
            rc(dc, dx, dz).wait_recv()
            value = value + from_core[dc - 1, dx, dz].astype(F32)
        return value

    for dx in range(1, nx):
        for dz in list(range(1, nz)) + [0]:
            summed[dx - 1, dz] = core_sum(dx, dz).astype(BF16)
            send(rx(dx, dz))
    own = None
    for dz in list(range(1, nz)) + [0]:
        value = core_sum(0, dz)
        for dx in range(1, nx):
            rx(dx, dz).wait_recv()
            value = value + from_x[dx - 1, dz].astype(F32)
        if dz > 0:
            to_z[dz - 1] = value.astype(BF16)
            send(rz(dz))
        else:
            own = value
    for dz in range(1, nz):
        rz(dz).wait_recv()
        own = own + from_z[dz - 1].astype(F32)
    for j in range(ntp):
        both = acc_buf[j] + own[:, j * cw : (j + 1) * cw]
        acc_buf[j] = both
        acc_send[j] = both.astype(BF16)

    def ry(dy):
        target = tp_at(dy)
        return remote(acc_send.at[target["tp"]], from_y.at[dy - 1], ry_s.at[dy - 1], ry_r.at[dy - 1], target)

    for dy in range(1, ntp):
        send(ry(dy))
    result = residual_buf[tp] + acc_buf[tp]
    for dy in range(1, ntp):
        ry(dy).wait_recv()
        result = result + from_y[dy - 1].astype(F32)
    out_ref[...] = result[:rows].astype(BF16)
    for copy in pending:
        copy.wait_send()


def local(
    sizes,
    tokens,
    norm_gain,
    w_query,
    w_key,
    w_value,
    w_input_gate,
    w_forget_gate,
    input_bias,
    forget_bias,
    state_c,
    state_n,
    state_m,
    w_mixer_out,
    ffn_gain,
    routes,
    route_scale,
    w_expert_gate,
    w_expert_up,
    w_expert_down,
    w_dense_gate,
    w_dense_up,
    w_dense_down,
    w_branch_gate,
):
    nz, nx, nc, ntp = sizes
    rows, width = tokens.shape
    heads = state_m.shape[1]
    value_size = state_c.shape[3]
    pad_rows = -(-rows // 16) * 16
    cw = width // ntp
    vmem = pl.BlockSpec(memory_space=pltpu.VMEM)
    hbm = pl.BlockSpec(memory_space=pl.ANY)
    dma = pltpu.SemaphoreType.DMA
    part, new_c, new_n, new_m = pl.pallas_call(
        cell_kernel,
        name="cell",
        out_shape=(
            jax.ShapeDtypeStruct((pad_rows, width), BF16),
            jax.ShapeDtypeStruct(state_c.shape, F32),
            jax.ShapeDtypeStruct(state_n.shape, F32),
            jax.ShapeDtypeStruct(state_m.shape[::-1], F32),
        ),
        in_specs=[hbm] * 13,
        out_specs=(vmem, hbm, vmem, vmem),
        scratch_shapes=[
            pltpu.VMEM(tokens.shape, BF16),
            pltpu.VMEM((1, width), F32),
            pltpu.VMEM(w_input_gate.shape[::-1], BF16),
            pltpu.VMEM(w_forget_gate.shape[::-1], BF16),
            pltpu.VMEM((1, input_bias.shape[0]), F32),
            pltpu.VMEM((1, forget_bias.shape[0]), F32),
            pltpu.VMEM(state_m.shape[::-1], F32),
            pltpu.VMEM(state_n.shape, F32),
            pltpu.VMEM(w_query.shape, BF16),
            pltpu.VMEM(w_key.shape, BF16),
            pltpu.VMEM(w_value.shape, BF16),
            pltpu.VMEM(state_c.shape, F32),
            pltpu.VMEM(state_c.shape, F32),
            pltpu.VMEM(w_mixer_out.shape, BF16),
            pltpu.VMEM((pad_rows, heads * value_size), F32),
            dma((11,)),
            dma((rows,)),
            dma((rows,)),
            dma,
        ],
        compiler_params=pltpu.CompilerParams(vmem_limit_bytes=VMEM_LIMIT),
    )(
        tokens,
        norm_gain.reshape(1, width),
        w_input_gate.T,
        w_forget_gate.T,
        input_bias.reshape(1, -1),
        forget_bias.reshape(1, -1),
        state_m.T,
        state_n,
        w_query,
        w_key,
        w_value,
        state_c,
        w_mixer_out,
    )
    block = (pad_rows, width)
    output = pl.pallas_call(
        functools.partial(ffn_kernel, sizes),
        name="ffn",
        out_shape=pltpu.VMEM((rows, cw), BF16),
        in_specs=[hbm] * 12,
        out_specs=vmem,
        scratch_shapes=[
            pltpu.VMEM(tokens.shape, BF16),
            pltpu.VMEM(block, BF16),
            pltpu.VMEM((1, width), F32),
            pltpu.VMEM(routes.shape[::-1], jnp.int32),
            pltpu.VMEM(route_scale.shape[::-1], BF16),
            pltpu.VMEM((width // 128, 128), BF16),
            pltpu.VMEM(w_expert_gate.shape[1:], BF16),
            pltpu.VMEM(w_expert_up.shape[1:], BF16),
            pltpu.VMEM(w_expert_down.shape[1:], BF16),
            pltpu.VMEM(w_dense_gate.shape, BF16),
            pltpu.VMEM(w_dense_up.shape, BF16),
            pltpu.VMEM(w_dense_down.shape, BF16),
            pltpu.VMEM((max(1, ntp - 1),) + block, BF16),
            pltpu.VMEM((nz * nx * nc, 1, 128), F32),
            pltpu.VMEM((nc, nx, nz) + block, BF16),
            pltpu.VMEM((nc, nx, nz, 1, 128), F32),
            pltpu.VMEM((nc, nx, nz) + block, BF16),
            pltpu.VMEM((max(1, nc - 1), nx, nz) + block, BF16),
            pltpu.VMEM((max(1, nx - 1), nz) + block, BF16),
            pltpu.VMEM((max(1, nx - 1), nz) + block, BF16),
            pltpu.VMEM((max(1, nz - 1),) + block, BF16),
            pltpu.VMEM((max(1, nz - 1),) + block, BF16),
            pltpu.VMEM((ntp, pad_rows, cw), F32),
            pltpu.VMEM((ntp, pad_rows, cw), F32),
            pltpu.VMEM((ntp, pad_rows, cw), BF16),
            pltpu.VMEM((max(1, ntp - 1), pad_rows, cw), BF16),
            dma((12,)),
            dma((max(1, ntp - 1),)),
            dma((max(1, ntp - 1),)),
            dma((nc, nx, nz)),
            dma((nc, nx, nz)),
            dma((nz,)),
            dma((nz,)),
            dma((nx, nz)),
            dma((nx, nz)),
            dma((nc, nx, nz)),
            dma((nc, nx, nz)),
            dma((nc, nx, nz)),
            dma((nc, nx, nz)),
            dma((nx, nz)),
            dma((nx, nz)),
            dma((nz,)),
            dma((nz,)),
            dma((max(1, ntp - 1),)),
            dma((max(1, ntp - 1),)),
        ],
        compiler_params=pltpu.CompilerParams(
            vmem_limit_bytes=VMEM_LIMIT, collective_id=0, has_side_effects=True
        ),
    )(
        tokens,
        part,
        ffn_gain.reshape(1, width),
        routes.T,
        route_scale.T,
        w_branch_gate.reshape(width // 128, 128),
        w_expert_gate,
        w_expert_up,
        w_expert_down,
        w_dense_gate,
        w_dense_up,
        w_dense_down,
    )
    return (output, new_c, new_n, new_m.T)


def solution(mesh):
    n_ep, n_tp = mesh.shape["ep"], mesh.shape["tp"]
    n_core = 2 if n_ep % 2 == 0 else 1
    n_x = n_tp if n_ep % (n_core * n_tp) == 0 else 1
    sizes = (n_ep // (n_core * n_x), n_x, n_core, n_tp)
    in_specs = (
        P("ep", None),
        P(),
        P(None, "tp"),
        P(None, "tp"),
        P(None, "tp"),
        P(),
        P(),
        P(),
        P(),
        P("ep", "tp", None, None),
        P("ep", "tp", None),
        P("ep", "tp"),
        P("tp", None),
        P(),
        P("ep", None),
        P("ep", None),
        P("ep", None, "tp"),
        P("ep", None, "tp"),
        P("ep", "tp", None),
        P(None, "tp"),
        P(None, "tp"),
        P("tp", None),
        P(),
    )
    out_specs = (P("ep", "tp"), P("ep", "tp", None, None), P("ep", "tp", None), P("ep", "tp"))
    return jax.shard_map(
        functools.partial(local, sizes),
        mesh=mesh,
        in_specs=in_specs,
        out_specs=out_specs,
        check_vma=False,
    )
```
